256 devices in a mesh: grp: 2 (over y), fs: 16 (over z), tp: 8 (over x, core).
Axes of the slice: x: 4, y: 2, z: 16, core: 2. Of those that a mesh axis runs over, the one named last changes fastest.
The devices are a block of a 4x16x16 slice.
Arguments:
- tokens: bfloat16 [32768, 2048], P(('grp', 'fs', 'tp')), parts along dimension 0, may hold values from -6 to 6
- mix_weight_in: bfloat16 [2048, 1024], P('fs', 'tp'), may hold values from -0.125 to 0.125
- pool_scale: float32 [1024], P('tp'), may hold values from 0.1 to 1.9
- mix_weight_out: bfloat16 [1024, 2048], P('tp', 'fs'), may hold values from -0.1875 to 0.1875
- up_weight: bfloat16 [2048, 8192], P('fs', 'tp'), may hold values from -0.125 to 0.125
- down_weight: bfloat16 [8192, 2048], P('tp', 'fs'), may hold values from -0.0625 to 0.0625
- gains: float32 [4, 2048], replicated, may hold values from 0.1 to 1.9
Outputs:
- result: bfloat16 [32768, 2048], P(('grp', 'fs', 'tp')), parts along dimension 0
The draws below stay inside these ranges and needn't reach their ends.
There are 2 independent parts, one for each index of `grp`. The reference program is written for one: setup_inputs(seed, part) draws one part's arguments, and reference() takes and returns one part's arrays. A program takes and returns all parts, laid end to end along the dimension named above; an argument that names none is the same for every part. Nothing has to cross between parts.
All inputs are finite; a program needn't handle non-finite values.
Results may differ from the reference program's by a relative error of at most 0.02.
Values may be sent and summed in bfloat16 or wider, within the bound.
A program may use at most 64 MiB of HBM per device.

```python
import jax
import jax.numpy as jnp
from jax import lax

D = 2048
PW = 1024
GROUPS = 4
FF = 8192
ROWS = 128
TOKENS = 16384
N_FS = 16
N_TP = 8


def level_of(own_key, extent, split, least, top_value):
    factor_of, own = 1.0, jax.random.fold_in(own_key, 6)
    for dim, blocks in split:
        heights = jnp.exp(jax.random.uniform(jax.random.fold_in(own, dim), (blocks,), jnp.float32, least / len(split), top_value / len(split)))
        factor_of = factor_of * jnp.repeat(heights, extent[dim] // blocks).reshape([-1 if axis == dim else 1 for axis in range(len(extent))])
    return factor_of


def scatter_about(key, shape, spread, reach, shards=(), kind=jnp.bfloat16):
    level = level_of(key, shape, shards, -0.22, 0.18) if shards else 1.0
    entries = jax.random.normal(key, shape, jnp.float32) * spread * level
    return jnp.minimum(jnp.maximum(entries, -reach), reach).astype(kind)


def setup_inputs(seed: int = 0, part: int = 0) -> dict:
    keys = jax.random.split(jax.random.key(seed), 8)
    own_keys = jax.random.split(jax.random.fold_in(keys[7], part), 8)
    return {
        "tokens": scatter_about(own_keys[0], (TOKENS, D), 1.0, 6.0, ((0, 128),)),
        "mix_weight_in": scatter_about(keys[1], (D, PW), D ** -0.5, 0.125, ((0, 16), (1, 8))),
        "pool_scale": jnp.clip(1.0 + 0.18 * jax.random.normal(keys[2], (PW,), jnp.float32), 0.1, 1.9),
        "mix_weight_out": scatter_about(keys[3], (PW, D), PW ** -0.5, 0.1875, ((0, 8), (1, 16))),
        "up_weight": scatter_about(keys[4], (D, FF), D ** -0.5, 0.125, ((0, 16), (1, 8))),
        "down_weight": scatter_about(keys[5], (FF, D), FF ** -0.5, 0.0625, ((0, 8), (1, 16))),
        "gains": jnp.clip(1.0 + 0.18 * jax.random.normal(keys[6], (4, D), jnp.float32), 0.1, 1.9),
    }


norm_eps = 1e-06
pool_spans = (2, 4, 8, 16)

def normalize(values, gain):
    upcast = values.astype(jnp.float32)
    return upcast * lax.rsqrt(lax.optimization_barrier(jnp.mean(upcast * upcast, axis=-1, keepdims=True)) + norm_eps) * gain

def pooling(mixed_in):
    length = mixed_in.shape[0]
    upcast = mixed_in.astype(jnp.float32)
    running = jnp.cumsum(upcast, axis=0)
    position = jnp.arange(1, length + 1, dtype=jnp.float32)[:, None]
    group_of = (jnp.arange(PW) // (PW // GROUPS))[None, :]
    average = jnp.zeros_like(upcast)
    for index, span in enumerate(pool_spans):
        lagged = jnp.pad(running, ((span, 0), (0, 0)))[:length]
        window_mean = (running - lagged) / jnp.minimum(position, float(span))
        average = jnp.where(group_of == index, window_mean, average)
    return average - upcast

def split_sum(left, right, width):
    total = jnp.zeros((left.shape[0], right.shape[1]), jnp.float32)
    for block in range(N_TP):
        partial_value = jnp.dot(left[:, block * width:(block + 1) * width], right[block * width:(block + 1) * width], preferred_element_type=jnp.float32)
        total = total + lax.optimization_barrier(partial_value.astype(jnp.bfloat16)).astype(jnp.float32)
    return total.astype(jnp.bfloat16)

def reference(tokens, mix_weight_in, pool_scale, mix_weight_out, up_weight, down_weight, gains):

    def one_sequence(sequence):
        normed = normalize(sequence, gains[0]).astype(jnp.bfloat16)
        mixed_in = jnp.dot(normed, mix_weight_in, preferred_element_type=jnp.float32).astype(jnp.bfloat16)
        scaled = (pooling(mixed_in) * pool_scale).astype(jnp.bfloat16)
        mixer_out = split_sum(scaled, mix_weight_out, PW // N_TP)
        middle = (sequence.astype(jnp.float32) + normalize(mixer_out, gains[1])).astype(jnp.bfloat16)
        normed_two = normalize(middle, gains[2]).astype(jnp.bfloat16)
        hidden_pre = jax.nn.relu(jnp.dot(normed_two, up_weight, preferred_element_type=jnp.float32))
        squared = (hidden_pre * hidden_pre).astype(jnp.bfloat16)
        channel_out = split_sum(squared, down_weight, FF // N_TP)
        return (middle.astype(jnp.float32) + normalize(channel_out, gains[3])).astype(jnp.bfloat16)
    sequences = tokens.reshape(N_FS, ROWS * N_TP, D)
    return lax.map(one_sequence, sequences).reshape(TOKENS, D)
```

```python
import functools

import jax
import jax.numpy as jnp
from jax import lax
from jax.experimental import pallas as pl
from jax.experimental.pallas import tpu as pltpu
from jax.sharding import PartitionSpec as P

PW = 1024
GROUPS = 4
EPS = 1e-06
MESH = pl.DeviceIdType.MESH
F32 = jnp.float32
BF16 = jnp.bfloat16


def rms(v):
    return v * lax.rsqrt(jnp.mean(v * v, axis=-1, keepdims=True) + EPS)


class Copies:
    def __init__(self, send, recv):
        self.send, self.recv, self.sent = send, recv, []

    def make(self, slot, src, dst, where):
        return pltpu.make_async_remote_copy(
            src_ref=src,
            dst_ref=dst,
            send_sem=self.send.at[slot],
            recv_sem=self.recv.at[slot],
            device_id=where,
            device_id_type=MESH,
        )

    def start(self, slot, src, dst, where):
        copy = self.make(slot, src, dst, where)
        copy.start()
        self.sent.append(copy)

    def arrived(self, slot, dst, where):
        self.make(slot, dst, dst, where).wait_recv()

    def drain(self):
        for copy in self.sent:
            copy.wait_send()


class Ring:
    def __init__(self, copies, own, place, me, n, hops, ends, mirror=None):
        self.copies, self.own, self.place = copies, own, place
        self.me, self.n, self.hops, self.ends = me, n, hops, ends
        self.mirror = mirror

    def slot(self, way, hop):
        return (self.hops[0] if way else 0) + hop - 1

    def origin(self, way, hop):
        return lax.rem(self.me + (hop if way else self.n - hop), self.n)

    def begin(self):
        for way in (0, 1):
            if self.hops[way]:
                self.copies.start(
                    self.slot(way, 1), self.own, self.place(self.me), self.ends[way]
                )

    def event(self, hop):
        for way in (0, 1):
            if hop > self.hops[way]:
                continue
            block = self.place(self.origin(way, hop))
            self.copies.arrived(self.slot(way, hop), block, self.ends[way])
            if hop < self.hops[way]:
                self.copies.start(
                    self.slot(way, hop + 1), block, block, self.ends[way]
                )
            if self.mirror:
                copies, partner, _ = self.mirror
                copies.start(self.slot(way, hop), block, block, partner)

    def mirrored(self):
        if self.mirror:
            copies, partner, other = self.mirror
            for way in (0, 1):
                for hop in range(1, self.hops[way] + 1):
                    copies.arrived(
                        self.slot(way, hop), other(self.origin(way, hop)), partner
                    )


def kernel(
    sizes,
    tok, gain, scale, w_in, w_out, w_up, w_down,
    out,
    xg1, xg2, b_in, b_out, b_up, b_down, mixed, scaled, sq, mid,
    part1, part2, dd1, dd2, rel1, rel2, fin1, fin2, sum1, sum2,
    own_sem, *sems,
):
    n_fs, n_tp, paired = sizes
    grp, z, t = lax.axis_index("grp"), lax.axis_index("fs"), lax.axis_index("tp")
    chips = n_tp // 2
    x, core = t // 2, lax.rem(t, 2)
    parity = lax.rem(grp, 2)
    chip_r, chip_l = lax.rem(x + 1, chips), lax.rem(x + chips - 1, chips)
    chip_o = lax.rem(x + 2, chips)
    east, west = {"tp": chip_r * 2 + core}, {"tp": chip_l * 2 + core}
    mate = {"tp": x * 2 + 1 - core}
    up_z, down_z = {"fs": lax.rem(z + 1, n_fs)}, {"fs": lax.rem(z + n_fs - 1, n_fs)}
    twin = {"grp": grp + 1 - 2 * parity}
    rows, width = tok.shape
    half = rows // 2

    barrier = pltpu.get_barrier_semaphore()
    greeted = [east, west, mate, up_z, down_z] + ([twin] if paired else [])
    for where in greeted:
        pl.semaphore_signal(barrier, inc=1, device_id=where, device_id_type=MESH)

    pairs = [Copies(sems[2 * i], sems[2 * i + 1]) for i in range(len(sems) // 2)]
    c_in, c_out, c_uo, c_um, c_do, c_dm, c_uy, c_dy, c_ag1, c_ag2, c_rs1, c_rs2 = pairs

    k_in, k_up = w_in.shape[0], w_up.shape[0]
    n_out, n_down = w_out.shape[1], w_down.shape[1]
    f_down = w_down.shape[0]

    def rows_of(buffer, depth, first, size):
        return lambda o: buffer.at[
            pl.ds(pl.multiple_of(o * depth + first, 16), size), :
        ]

    def cols_of(buffer, depth, first, size):
        return lambda o: buffer.at[
            pl.ds(pl.multiple_of(first, 16), size),
            pl.ds(pl.multiple_of(o * depth, 128), depth),
        ]

    local = [
        pltpu.make_async_copy(w_in, rows_of(b_in, k_in, 0, k_in)(z), own_sem.at[0]),
        pltpu.make_async_copy(
            w_out, cols_of(b_out, n_out, 0, w_out.shape[0])(z), own_sem.at[1]
        ),
        pltpu.make_async_copy(w_up, rows_of(b_up, k_up, 0, k_up)(z), own_sem.at[2]),
        pltpu.make_async_copy(
            w_down, cols_of(b_down, n_down, 0, f_down)(z), own_sem.at[3]
        ),
    ]
    for copy in local:
        copy.start()

    big, small = n_fs // 2, n_fs - 1 - n_fs // 2
    ends = (up_z, down_z)
    if paired:
        outer_k, inner_k = 3 * k_up // 8, 2 * k_up // 8
        outer_f, inner_f = 3 * f_down // 8, 2 * f_down // 8
    else:
        outer_k, inner_k = k_up // 2, k_up // 2
        outer_f, inner_f = f_down // 2, f_down // 2

    def part_of(outer, inner):
        if paired:
            step = outer + inner
            return parity * step, outer, (1 - parity) * step
        return 0, inner, 0

    uo, um, uy = part_of(outer_k, inner_k)
    do, dm, dy = part_of(outer_f, inner_f)

    def own_rows(ref, first, size):
        return ref.at[pl.ds(pl.multiple_of(first, 16), size), :]

    ring = functools.partial(Ring, me=z, n=n_fs, ends=ends)
    r_in = ring(c_in, w_in, rows_of(b_in, k_in, 0, k_in), hops=(big, small))
    r_out = ring(
        c_out, w_out, cols_of(b_out, n_out, 0, w_out.shape[0]), hops=(small, big)
    )
    r_uo = ring(
        c_uo, own_rows(w_up, uo, outer_k), rows_of(b_up, k_up, uo, outer_k),
        hops=(big, small),
        mirror=(c_uy, twin, rows_of(b_up, k_up, uy, outer_k)) if paired else None,
    )
    r_um = ring(
        c_um, own_rows(w_up, um, inner_k), rows_of(b_up, k_up, um, inner_k),
        hops=(small, big),
    )
    r_do = ring(
        c_do, own_rows(w_down, do, outer_f), cols_of(b_down, n_down, do, outer_f),
        hops=(big, small),
        mirror=(c_dy, twin, cols_of(b_down, n_down, dy, outer_f)) if paired else None,
    )
    r_dm = ring(
        c_dm, own_rows(w_down, dm, inner_f), cols_of(b_down, n_down, dm, inner_f),
        hops=(small, big),
    )

    def mix_event(hop):
        r_in.event(hop)
        r_out.event(hop)

    def begin_down():
        r_do.begin()
        r_dm.begin()

    todo = []
    for hop in range(1, big + 1):
        todo.append(functools.partial(mix_event, hop))
        todo.append(functools.partial((r_uo, r_um)[(hop - 1) % 2].event, (hop + 1) // 2))
    reached = (big + 1) // 2
    todo.append(begin_down)
    lag = reached
    for hop in range(reached + 1, big + 1):
        todo += [functools.partial(r_uo.event, hop), functools.partial(r_um.event, hop)]
        todo += [functools.partial(r_do.event, hop - lag), functools.partial(r_dm.event, hop - lag)]
    for hop in range(big - lag + 1, big + 1):
        todo += [functools.partial(r_do.event, hop), functools.partial(r_dm.event, hop)]

    def pump(count):
        for _ in range(count):
            if todo:
                todo.pop(0)()

    def block(buffer, tp, part=None):
        first, size = (0, rows) if part is None else (part * half, half)
        return buffer.at[pl.ds(pl.multiple_of(tp * rows + first, 16), size), :]

    t_w, t_e, t_o = chip_l * 2 + core, chip_r * 2 + core, chip_o * 2 + core
    flip = 1 - 2 * core

    class Gather:
        def __init__(self, copies, buffer):
            self.c, self.b = copies, buffer

        def begin(self):
            c, b = self.c, self.b
            c.start(0, block(b, t, 0), block(b, t, 0), east)
            c.start(3, block(b, t, 1), block(b, t, 1), west)
            c.start(1, block(b, t, 1), block(b, t, 1), east)
            c.start(4, block(b, t, 0), block(b, t, 0), west)
            c.start(6, block(b, t), block(b, t), mate)

        def got_mate(self):
            self.c.arrived(6, block(self.b, t + flip), mate)

        def got(self, slot, tp, part, where, relay=None):
            c, piece = self.c, block(self.b, tp, part)
            c.arrived(slot, piece, where)
            if relay is not None:
                c.start(relay, piece, piece, east if relay == 2 else west)
            c.start(7 + slot, piece, piece, mate)

        def first(self):
            self.got(0, t_w, 0, west, 2)
            self.got(3, t_e, 1, east, 5)

        def second(self):
            self.got(1, t_w, 1, west)
            self.got(4, t_e, 0, east)

        def third(self):
            self.got(2, t_o, 0, west)
            self.got(5, t_o, 1, east)

        def mates_near(self):
            for slot, tp, part in ((0, t_w, 0), (3, t_e, 1), (1, t_w, 1), (4, t_e, 0)):
                self.c.arrived(7 + slot, block(self.b, tp + flip, part), mate)

        def mates_far(self):
            for slot, part in ((2, 0), (5, 1)):
                self.c.arrived(7 + slot, block(self.b, t_o + flip, part), mate)

    dest = (chip_o, chip_r, chip_l, x)

    def lines(count, body, step=16):
        @pl.loop(0, count // step)
        def _(i):
            body(pl.ds(pl.multiple_of(i * step, step), step))

    class Sum:
        def __init__(self, copies, part, dd, rel, fin, total):
            self.c, self.part, self.dd = copies, part, dd
            self.rel, self.fin, self.total = rel, fin, total

        def give(self, i):
            self.c.start(
                i, block(self.part, dest[i] * 2 + 1 - core), self.dd.at[i], mate
            )

        def add(self, i):
            self.c.arrived(i, self.dd.at[i], mate)
            base = (dest[i] * 2 + core) * rows

            def body(at):
                mine = self.part[pl.ds(pl.multiple_of(base + at.start, 16), 16), :]
                both = mine.astype(F32) + self.dd[i, at, :].astype(F32)
                self.total[i, at, :] = both.astype(BF16)

            lines(rows, body)

        def half_of(self, i, h):
            return self.total.at[i, pl.ds(h * half, half), :]

        def far(self):
            self.add(0)
            self.c.start(4, self.half_of(0, 0), self.rel.at[0], east)
            self.c.start(5, self.half_of(0, 1), self.rel.at[1], west)

        def near(self):
            self.add(1)
            self.c.start(
                6, self.half_of(1, 1), self.fin.at[0, pl.ds(half, half), :], east
            )
            self.add(2)
            self.c.start(
                7, self.half_of(2, 0), self.fin.at[1, pl.ds(0, half), :], west
            )

        def relay(self):
            for way, i, h, where, back in ((0, 1, 0, east, west), (1, 2, 1, west, east)):
                self.c.arrived(4 + way, self.rel.at[way], back)

                def body(at):
                    to = pl.ds(pl.multiple_of(h * half + at.start, 16), 16)
                    both = self.total[i, to, :].astype(F32) + self.rel[way, at, :].astype(F32)
                    self.total[i, to, :] = both.astype(BF16)

                lines(half, body)
                self.c.start(
                    8 + way,
                    self.half_of(i, h),
                    self.fin.at[way, pl.ds(h * half, half), :],
                    where,
                )

        def own(self):
            self.c.arrived(3, self.dd.at[3], mate)

        def final_near(self):
            self.c.arrived(6, self.fin.at[0, pl.ds(half, half), :], west)
            self.c.arrived(7, self.fin.at[1, pl.ds(0, half), :], east)

        def final(self):
            self.c.arrived(8, self.fin.at[0, pl.ds(0, half), :], west)
            self.c.arrived(9, self.fin.at[1, pl.ds(half, half), :], east)

        def result(self, at):
            mine = self.part[pl.ds(pl.multiple_of(t * rows + at.start, 16), 16), :]
            total = mine.astype(F32) + self.dd[3, at, :].astype(F32)
            total += self.fin[0, at, :].astype(F32)
            total += self.fin[1, at, :].astype(F32)
            return total.astype(BF16).astype(F32)

    g1, g2 = Gather(c_ag1, xg1), Gather(c_ag2, xg2)
    s1 = Sum(c_rs1, part1, dd1, rel1, fin1, sum1)
    s2 = Sum(c_rs2, part2, dd2, rel2, fin2, sum2)

    def gain_row(i):
        return gain[pl.ds(i, 1), :]

    def first_norm(at):
        y = rms(tok[at, :].astype(F32)) * gain_row(0)
        xg1[pl.ds(pl.multiple_of(t * rows + at.start, 16), 16), :] = y.astype(BF16)

    lines(rows, first_norm)
    mixed[pl.ds(0, 16), :] = jnp.zeros((16, mixed.shape[1]), F32)

    pl.semaphore_wait(barrier, len(greeted))
    r_in.begin()
    r_out.begin()
    g1.begin()
    r_uo.begin()
    r_um.begin()
    for copy in local:
        copy.wait()

    pair = 2 * rows

    def chip_rows(chip):
        return pl.ds(pl.multiple_of(chip * pair, 16), pair)

    pump(2)
    g1.got_mate()
    pump(2)
    g1.first()
    pump(4)
    g1.second()
    pump(2)
    g1.mates_near()
    g1.third()
    pump(4)
    g1.mates_far()
    pump(2 * big - 14)

    @pl.loop(0, chips)
    def _(i):
        y = jnp.dot(xg1[chip_rows(i), :], b_in[...], preferred_element_type=F32)
        mixed[pl.ds(pl.multiple_of(i * pair + 16, 16), pair), :] = y.astype(BF16).astype(F32)

    channels = mixed.shape[1]
    lane = lax.broadcasted_iota(jnp.int32, (1, channels), 1)
    group = (t * channels + lane) // (PW // GROUPS)
    span = jnp.where(group == 0, 2, jnp.where(group == 1, 4, jnp.where(group == 2, 8, 16)))

    @pl.loop(0, n_tp)
    def _(i):
        v = mixed[pl.ds(pl.multiple_of(i * rows, 16), rows + 16), :]
        two = v + pltpu.roll(v, 1, 0)
        four = two + pltpu.roll(two, 2, 0)
        eight = four + pltpu.roll(four, 4, 0)
        sixteen = eight + pltpu.roll(eight, 8, 0)
        total = jnp.where(group == 0, two, jnp.where(group == 1, four, jnp.where(group == 2, eight, sixteen)))
        total, v = total[16:, :], v[16:, :]
        position = i * rows + 1 + lax.broadcasted_iota(jnp.int32, (rows, channels), 0)
        count = jnp.minimum(position, span).astype(F32)
        y = (total / count - v) * scale[...]
        scaled[pl.ds(pl.multiple_of(i * rows, 16), rows), :] = y.astype(BF16)

    tile = 256

    def mix_back(chip):
        @pl.loop(0, width // tile)
        def _(j):
            at = pl.ds(pl.multiple_of(j * tile, tile), tile)
            y = jnp.dot(scaled[chip_rows(chip), :], b_out[:, at], preferred_element_type=F32)
            part1[chip_rows(chip), at] = y.astype(BF16)

    mix_back(chip_o)
    s1.give(0)
    mix_back(chip_r)
    s1.give(1)
    s1.far()
    mix_back(chip_l)
    s1.give(2)
    s1.near()
    mix_back(x)
    s1.give(3)
    pump(4)
    s1.relay()
    s1.own()
    pump(4)
    s1.final_near()
    pump(3)
    s1.final()

    def second_norm(at):
        m = tok[at, :].astype(F32) + rms(s1.result(at)) * gain_row(1)
        m = m.astype(BF16)
        mid[at, :] = m
        y = rms(m.astype(F32)) * gain_row(2)
        xg2[pl.ds(pl.multiple_of(t * rows + at.start, 16), 16), :] = y.astype(BF16)

    lines(rows, second_norm)
    g2.begin()
    pump(4)
    g2.got_mate()
    g2.first()
    pump(3)
    g2.second()
    g2.mates_near()
    pump(3)

    def expand(chip):
        @pl.loop(0, sq.shape[1] // tile)
        def _(j):
            at = pl.ds(pl.multiple_of(j * tile, tile), tile)
            h = jnp.dot(xg2[chip_rows(chip), :], b_up[:, at], preferred_element_type=F32)
            h = jnp.maximum(h, 0.0)
            sq[chip_rows(chip), at] = (h * h).astype(BF16)

    def contract(chip):
        @pl.loop(0, width // tile)
        def _(j):
            at = pl.ds(pl.multiple_of(j * tile, tile), tile)
            y = jnp.dot(sq[chip_rows(chip), :], b_down[:, at], preferred_element_type=F32)
            part2[chip_rows(chip), at] = y.astype(BF16)

    g2.third()
    r_uo.mirrored()
    expand(x)
    pump(2)
    expand(chip_l)
    pump(2)
    expand(chip_r)
    g2.mates_far()
    pump(2)
    expand(chip_o)
    pump(len(todo))
    r_do.mirrored()

    contract(chip_o)
    s2.give(0)
    contract(chip_r)
    s2.give(1)
    s2.far()
    contract(chip_l)
    s2.give(2)
    s2.near()
    contract(x)
    s2.give(3)
    s2.relay()
    s2.own()
    s2.final_near()
    s2.final()

    def last_norm(at):
        y = mid[at, :].astype(F32) + rms(s2.result(at)) * gain_row(3)
        out[at, :] = y.astype(BF16)

    lines(rows, last_norm)
    for copies in pairs:
        copies.drain()


def solution(mesh):
    n_fs, n_tp = mesh.shape["fs"], mesh.shape["tp"]
    paired = mesh.shape["grp"] % 2 == 0

    def layer(tokens, mix_in, pool_scale, mix_out, up, down, gains):
        rows, width = tokens.shape
        channels, hidden = mix_in.shape[1], up.shape[1]
        seq = rows * n_tp
        vmem = pl.BlockSpec(memory_space=pltpu.VMEM)
        far = pl.BlockSpec(memory_space=pl.ANY)
        sems = []
        for count in [n_fs - 1] * 8 + [13, 13, 10, 10]:
            sems += [pltpu.SemaphoreType.DMA((count,))] * 2
        sums = lambda *lead: pltpu.VMEM((*lead, width), BF16)
        return pl.pallas_call(
            functools.partial(kernel, (n_fs, n_tp, paired)),
            out_shape=jax.ShapeDtypeStruct((rows, width), BF16),
            in_specs=[vmem, vmem, vmem, far, far, far, far],
            out_specs=vmem,
            scratch_shapes=[
                sums(seq), sums(seq),
                pltpu.VMEM((width, channels), BF16),
                sums(channels),
                pltpu.VMEM((width, hidden), BF16),
                sums(hidden),
                pltpu.VMEM((seq + 16, channels), F32),
                pltpu.VMEM((seq, channels), BF16),
                pltpu.VMEM((seq, hidden), BF16),
                sums(rows),
                sums(seq), sums(seq),
                sums(4, rows), sums(4, rows),
                sums(2, rows // 2), sums(2, rows // 2),
                sums(2, rows), sums(2, rows),
                sums(3, rows), sums(3, rows),
                pltpu.SemaphoreType.DMA((4,)),
                *sems,
            ],
            compiler_params=pltpu.CompilerParams(
                collective_id=0,
                has_side_effects=True,
                vmem_limit_bytes=60 * 1024 * 1024,
            ),
            name="layer",
        )(tokens, gains, pool_scale.reshape(1, -1), mix_in, mix_out, up, down)

    spread = P(("grp", "fs", "tp"), None)
    return jax.shard_map(
        layer,
        mesh=mesh,
        in_specs=(
            spread,
            P("fs", "tp"),
            P("tp"),
            P("tp", "fs"),
            P("fs", "tp"),
            P("tp", "fs"),
            P(),
        ),
        out_specs=spread,
        check_vma=False,
    )
```

```python
import contextlib
import functools
import math

import jax
import jax.numpy as jnp
from jax import lax
from jax.experimental import pallas as pl
from jax.experimental.pallas import tpu as pltpu
from jax.sharding import PartitionSpec as P

PW = 1024
GROUPS = 4
EPS = 1e-06
CUTS = (4, 6)
MIX_TIMES = (9.0, 12.5, 16.0, 20.0)
UO_BEGIN, UM_BEGIN, DOWN_BEGIN, MIX_DONE = 4.2, 9.2, 24.7, 24.9
UO_TIMES = (16.5, 22.5, 28.2, 33.5, 38.6, 43.6, 49.8, 53.5)
UM_TIMES = (18.0, 24.0, 29.6, 34.5, 39.4, 44.4, 50.5, 54.3)
DOWN_TIMES = (34.8, 44.8, 52.5, 57.5, 62.5, 66.8, 70.9, 73.9)
LAST_TIMES = (
    (68.8, 69.5, 70.2, 71.0, 71.8, 77.6),
    (73.0, 73.5, 74.0, 74.5, 75.4, 80.1),
    (79.5, 79.7, 79.8, 79.9, 80.0, 82.5),
)
MESH = pl.DeviceIdType.MESH
F32 = jnp.float32
BF16 = jnp.bfloat16


def scope(name):
    return contextlib.nullcontext()


def rms(v):
    return v * lax.rsqrt(jnp.mean(v * v, axis=-1, keepdims=True) + EPS)


class Copies:
    def __init__(self, name, send, recv, spare):
        self.name, self.send, self.recv, self.spare = name, send, recv, spare
        self.together = recv.shape[0] == 1
        self.begun, self.size = set(), 0

    def make(self, slot, src, dst, where):
        return pltpu.make_async_remote_copy(
            src_ref=src,
            dst_ref=dst,
            send_sem=self.send.at[0],
            recv_sem=self.recv.at[0 if self.together else slot],
            device_id=where,
            device_id_type=MESH,
        )

    def start(self, slot, src, dst, where):
        self.make(slot, src, dst, where).start()
        self.begun.add(slot)
        self.size += math.prod(src.shape)

    def arrived(self, slot, dst, where):
        assert slot in self.begun, (self.name, slot)
        with scope(f"{self.name}_{slot}"):
            self.make(slot, dst, dst, where).wait_recv()

    def all_of(self):
        for ref in self.spare:
            lines, rest = divmod(self.size, ref.shape[1])
            if rest == 0 and lines % 16 == 0 and lines <= ref.shape[0]:
                return ref.at[pl.ds(0, lines), :]
        raise ValueError(self.name)

    def arrived_all(self, where):
        with scope(f"{self.name}_all"):
            every = self.all_of()
            self.make(0, every, every, where).wait_recv()

    def drain(self, where):
        every = self.all_of()
        self.make(0, every, every, where).wait_send()


class Ring:
    def __init__(self, copies, own, place, me, n, hops, ends, mirror=None):
        self.copies, self.own, self.place = copies, own, place
        self.me, self.n, self.hops, self.ends = me, n, hops, ends
        self.mirror = mirror

    def slot(self, way, hop):
        return (self.hops[0] if way else 0) + hop - 1

    def block(self, way, hop):
        step = hop if way else self.n - hop
        return self.place(lax.rem(self.me + step, self.n))

    def send(self, way, hop, src, dst, reach=1):
        if hop <= self.hops[way]:
            where = self.ends[reach - 1][way]
            self.copies.start(self.slot(way, hop), src, dst, where)

    def take(self, way, hop, reach=1):
        block = self.block(way, hop)
        self.copies.arrived(self.slot(way, hop), block, self.ends[reach - 1][way])
        return block

    def onward(self, way, hop, block):
        return block

    def reflect(self, way, hop, block):
        if self.mirror:
            copies, partner = self.mirror
            copies.start(self.slot(way, hop), block, block, partner)

    def begin(self):
        for way in (0, 1):
            self.send(way, 1, self.own, self.onward(way, 1, self.place(self.me)))

    def event(self, hop, later=False):
        for way in (0, 1):
            if hop <= self.hops[way]:
                block = self.take(way, hop)
                self.send(way, hop + 1, block, self.onward(way, hop + 1, block))
                if not later:
                    self.reflect(way, hop, block)

    def reflect_both(self, hop):
        for way in (0, 1):
            if hop <= self.hops[way]:
                self.reflect(way, hop, self.block(way, hop))

    def mirrored(self):
        if self.mirror:
            copies, partner = self.mirror
            assert len(copies.begun) == sum(self.hops)
            copies.arrived_all(partner)


class Arrivals(Ring):
    def __init__(self, *args, cuts=None):
        super().__init__(*args)
        self.cuts = (*cuts, self.n)

    def block(self, way, hop):
        return self.place(min(2 * hop - 1 + way, self.n - 1))

    def onward(self, way, hop, block):
        return self.block(way, hop) if hop <= self.hops[way] else block

    def group(self, hop):
        return sum(hop > cut for cut in self.cuts)

    def reflect(self, way, hop, block):
        if self.mirror:
            copies, partner = self.mirror
            copies = copies[self.group(hop)]
            copies.start(self.slot(way, hop), block, block, partner)

    def mirrored(self, group):
        if self.mirror:
            copies, partner = self.mirror
            hops = [h for way in (0, 1) for h in range(1, self.hops[way] + 1)]
            count = sum(self.group(h) == group for h in hops)
            assert len(copies[group].begun) == count
            copies[group].arrived_all(partner)


class Leaps(Ring):
    def begin(self):
        for way in (0, 1):
            self.send(way, 2, self.own, self.place(self.me), 2)
        for way in (0, 1):
            self.send(way, 1, self.own, self.place(self.me))

    def event(self, leap):
        hop = 2 * leap
        blocks = [None, None]
        for way in (0, 1):
            if hop <= self.hops[way]:
                blocks[way] = self.take(way, hop, 2)
                self.send(way, hop + 2, blocks[way], blocks[way], 2)
        for way in (0, 1):
            if blocks[way] is not None:
                self.send(way, hop + 1, blocks[way], blocks[way])
                self.reflect(way, hop, blocks[way])
        for way in (0, 1):
            if hop - 1 <= self.hops[way]:
                self.reflect(way, hop - 1, self.take(way, hop - 1))


def lines(first, count, body, step=16, unroll=4):
    @pl.loop(0, count // step, unroll=unroll)
    def _(i):
        body(pl.ds(pl.multiple_of(first + i * step, step), step))


class Gather:
    def __init__(self, copies, buffer, rows, place):
        self.c, self.buffer, self.rows = copies, buffer, rows
        self.t, self.t_w, self.t_e, self.t_o, self.flip = place[:5]
        self.east, self.west, self.mate = place[5:]

    def piece(self, tp, first, size):
        unit = self.rows // 4
        start = pl.multiple_of(tp * self.rows + first * unit, 16)
        return self.buffer.at[pl.ds(start, size * unit), :]

    def begin(self, h):
        for k, way in ((0, 0), (1, 1), (1, 0), (0, 1)):
            q = 2 * h + k
            piece = self.piece(self.t, q, 1)
            self.c.start(4 * way + q, piece, piece, self.west if way else self.east)
        piece = self.piece(self.t, 2 * h, 2)
        self.c.start(12 + h, piece, piece, self.mate)

    def take(self, slot, tp, q, way):
        where = self.east if way else self.west
        self.c.arrived(slot, self.piece(tp, q, 1), where)

    def hand(self, slot, tp, h):
        piece = self.piece(tp, 2 * h, 2)
        self.c.start(slot, piece, piece, self.mate)

    def near(self, h):
        for way, tp, k in ((0, self.t_w, 0), (1, self.t_e, 1)):
            q = 2 * h + k
            self.take(4 * way + q, tp, q, way)
            piece = self.piece(tp, q, 1)
            self.c.start(
                8 + 2 * way + h, piece, piece, self.west if way else self.east
            )
        for way, tp, k in ((0, self.t_w, 1), (1, self.t_e, 0)):
            q = 2 * h + k
            self.take(4 * way + q, tp, q, way)
            self.hand(14 + 2 * way + h, tp, h)

    def far(self, h):
        for way in (0, 1):
            self.take(8 + 2 * way + h, self.t_o, 2 * h + way, way)
        self.hand(18 + h, self.t_o, h)

    def from_mate(self, slot, tp, h):
        self.c.arrived(slot, self.piece(tp + self.flip, 2 * h, 2), self.mate)

    def mate_own(self):
        for h in (0, 1):
            self.from_mate(12 + h, self.t, h)

    def mate_near(self):
        for way, tp in ((0, self.t_w), (1, self.t_e)):
            for h in (0, 1):
                self.from_mate(14 + 2 * way + h, tp, h)

    def mate_far(self):
        for h in (0, 1):
            self.from_mate(18 + h, self.t_o, h)


class Sum:
    def __init__(self, copies, bufs, rows, dest, core, ways, cols):
        self.c, self.rows, self.dest, self.core = copies, rows, dest, core
        self.part, self.dd, self.rel, self.fin, self.total = bufs
        self.east, self.west, self.mate = ways
        self.unit, self.cols = rows // 4, cols

    def base(self, i, core):
        return (self.dest[i] * 2 + core) * self.rows

    def give(self, i):
        start = pl.multiple_of(self.base(i, 1 - self.core), 16)
        piece = self.part.at[pl.ds(start, self.rows), self.cols]
        self.c.start(i, piece, self.dd.at[i, :, self.cols], self.mate)

    def add(self, i):
        self.c.arrived(i, self.dd.at[i, :, self.cols], self.mate)
        base, cols = self.base(i, self.core), self.cols

        def body(at):
            mine = self.part[pl.ds(pl.multiple_of(base + at.start, 16), 16), cols]
            both = mine.astype(F32) + self.dd[i, at, cols].astype(F32)
            self.total[i, at, cols] = both.astype(BF16)

        lines(0, self.rows, body)

    def quarter(self, ref, i, q):
        return ref.at[i, pl.ds(q * self.unit, self.unit), self.cols]

    def far(self, way):
        for k in (0, 1):
            self.c.start(
                4 + 2 * way + k,
                self.quarter(self.total, 0, 2 * k + way),
                self.quarter(self.rel, way, k),
                self.west if way else self.east,
            )

    def direct(self, way):
        for k in (0, 1):
            q = 2 * k + 1 - way
            self.c.start(
                8 + 2 * way + k,
                self.quarter(self.total, 1 + way, q),
                self.quarter(self.fin, way, q),
                self.west if way else self.east,
            )

    def relay(self, way, k):
        there, back = (self.west, self.east) if way else (self.east, self.west)
        self.c.arrived(4 + 2 * way + k, self.quarter(self.rel, way, k), back)
        q, cols = 2 * k + way, self.cols
        shift = (q - k) * self.unit

        def body(at):
            to = pl.ds(pl.multiple_of(at.start + shift, 16), 16)
            both = self.total[1 + way, to, cols].astype(F32)
            both += self.rel[way, at, cols].astype(F32)
            self.total[1 + way, to, cols] = both.astype(BF16)

        lines(k * self.unit, self.unit, body)
        self.c.start(
            12 + 2 * way + k,
            self.quarter(self.total, 1 + way, q),
            self.quarter(self.fin, way, q),
            there,
        )

    def own(self):
        self.c.arrived(3, self.dd.at[3, :, self.cols], self.mate)

    def finish(self, h):
        for slot, way, q in (
            (8 + h, 0, 2 * h + 1),
            (10 + h, 1, 2 * h),
            (12 + h, 0, 2 * h),
            (14 + h, 1, 2 * h + 1),
        ):
            back = self.east if way else self.west
            self.c.arrived(slot, self.quarter(self.fin, way, q), back)

    def result(self, at):
        base = self.base(3, self.core)
        mine = self.part[pl.ds(pl.multiple_of(base + at.start, 16), 16), :]
        total = mine.astype(F32) + self.dd[3, at, :].astype(F32)
        total += self.fin[0, at, :].astype(F32)
        total += self.fin[1, at, :].astype(F32)
        return total.astype(BF16).astype(F32)


NAMES = ("in", "out", "iy", "oy", "uo", "um", "uy", "do", "dm", "dx", "dy", "dz", "ag", "ah", "rs", "rt", "ru", "rv")


def kernel(
    sizes,
    tokens, gain, scale, w_in, w_out, w_up, w_down,
    out,
    tok, xg1, xg2, b_in, b_out, b_up, b_down, mixed, scaled, sq, mid, last,
    part1, part2, dd1, dd2, rel1, rel2, fin1, fin2, sum1, sum2,
    own_sem, *sems,
):
    n_fs, n_tp, paired = sizes
    grp, z, t = lax.axis_index("grp"), lax.axis_index("fs"), lax.axis_index("tp")
    chips = n_tp // 2
    x, core = t // 2, lax.rem(t, 2)
    parity = lax.rem(grp, 2)
    chip_r, chip_l = lax.rem(x + 1, chips), lax.rem(x + chips - 1, chips)
    chip_o = lax.rem(x + 2, chips)
    east, west = {"tp": chip_r * 2 + core}, {"tp": chip_l * 2 + core}
    mate = {"tp": x * 2 + 1 - core}
    ends = tuple(
        tuple({"fs": lax.rem(z + d, n_fs)} for d in (k, n_fs - k)) for k in (1, 2)
    )
    twin = {"grp": grp + 1 - 2 * parity}
    rows, width = tok.shape
    half = rows // 2

    barrier = pltpu.get_barrier_semaphore()
    greeted = [east, west, mate, *ends[0], *ends[1]] + ([twin] if paired else [])
    for where in greeted:
        pl.semaphore_signal(barrier, inc=1, device_id=where, device_id_type=MESH)

    spare = (xg1, b_up, b_in)
    pairs = [Copies(n, sems[2 * i], sems[2 * i + 1], spare) for i, n in enumerate(NAMES)]
    c_in, c_out, c_iy, c_oy, c_uo, c_um, c_uy, c_do, c_dm = pairs[:9]
    c_dys, (c_ag1, c_ag2, c_rs1), c_last = pairs[9:12], pairs[12:15], pairs[15:]

    k_in, k_up, k_out = w_in.shape[0], w_up.shape[0], w_out.shape[0]
    n_out, n_down, f_down = w_out.shape[1], w_down.shape[1], w_down.shape[0]

    def rows_of(buffer, depth, first, size):
        return lambda o: buffer.at[
            pl.ds(pl.multiple_of(o * depth + first, 16), size), :
        ]

    def cols_of(buffer, depth, first, size):
        return lambda o: buffer.at[
            pl.ds(pl.multiple_of(first, 16), size),
            pl.ds(pl.multiple_of(o * depth, 128), depth),
        ]

    fetch = pltpu.make_async_copy(tokens, tok, own_sem.at[4])
    fetch.start()

    big, small = n_fs // 2, n_fs - 1 - n_fs // 2

    def make(kind, copies, shard, of, buffer, depth, first, size, hops, mirror):
        own = shard.at[pl.ds(pl.multiple_of(first, 16), size), :]
        place = of(buffer, depth, first, size)
        if mirror is not None:
            mirror = (mirror[0], twin)
        return kind(copies, own, place, z, n_fs, hops, ends, mirror)

    def split(depth, eighths):
        if not paired:
            return (0, depth // 2), (depth // 2, depth // 2), None
        outer = eighths * depth // 8
        inner = depth - 2 * outer
        skip = outer + inner
        return (parity * skip, outer), (outer, inner), (1 - parity) * skip

    def halves(depth):
        if not paired:
            return 0, depth, None
        return parity * (depth // 2), depth // 2, (1 - parity) * (depth // 2)

    def mirror(copies, first):
        return None if first is None else (copies, first)

    far_e, far_w = (big, small), (small, big)
    f, size, m = halves(k_in)
    r_in = make(Leaps, c_in, w_in, rows_of, b_in, k_in, f, size, far_e, mirror(c_iy, m))
    f, size, m = halves(k_out)
    r_out = make(Leaps, c_out, w_out, cols_of, b_out, n_out, f, size, far_w, mirror(c_oy, m))
    outer, inner, m = split(k_up, 3)
    r_uo = make(Ring, c_uo, w_up, rows_of, b_up, k_up, *outer, far_e, mirror(c_uy, m))
    r_um = make(Ring, c_um, w_up, rows_of, b_up, k_up, *inner, far_w, None)
    outer, inner, m = split(f_down, 2)
    kind = functools.partial(Arrivals, cuts=CUTS)
    r_do = make(kind, c_do, w_down, cols_of, b_down, n_down, *outer, far_e, mirror(c_dys, m))
    r_dm = make(kind, c_dm, w_down, cols_of, b_down, n_down, *inner, far_w, None)

    due = []

    def at_time(when, *steps):
        for step in steps:
            due.append((when, len(due), step))

    step = functools.partial

    def due_at(times, k):
        if k < len(times):
            return times[k]
        return times[-1] + (k + 1 - len(times)) * (times[-1] - times[-2])

    for leap in range((big + 1) // 2):
        at_time(due_at(MIX_TIMES, leap), step(r_in.event, leap + 1), step(r_out.event, leap + 1))
    at_time(UO_BEGIN, r_uo.begin)
    at_time(UM_BEGIN, r_um.begin)
    at_time(DOWN_BEGIN, r_do.begin, r_dm.begin)
    for hop in range(1, big + 1):
        when = due_at(UO_TIMES, hop - 1)
        at_time(when, step(r_uo.event, hop, when < MIX_DONE))
        if when < MIX_DONE:
            at_time(MIX_DONE, step(r_uo.reflect_both, hop))
        at_time(due_at(UM_TIMES, hop - 1), step(r_um.event, hop))
        when = due_at(DOWN_TIMES, hop - 1)
        at_time(when, step(r_do.event, hop))
        at_time(when + 0.4, step(r_dm.event, hop))

    ways = (east, west, mate)
    place = (t, chip_l * 2 + core, chip_r * 2 + core, chip_o * 2 + core, 1 - 2 * core)
    dest = (chip_o, chip_r, chip_l, x)
    g1 = Gather(c_ag1, xg1, rows, place + ways)
    g2 = Gather(c_ag2, xg2, rows, place + ways)
    s1 = Sum(c_rs1, (part1, dd1, rel1, fin1, sum1), rows, dest, core, ways, pl.ds(0, width))
    bufs = (part2, dd2, rel2, fin2, sum2)
    bounds = [0] + [(2 * cut + 1) * n_down for cut in CUTS] + [width]
    lasts = [
        Sum(copies, bufs, rows, dest, core, ways, pl.ds(low, high - low))
        for copies, low, high in zip(c_last, bounds, bounds[1:])
    ]

    def gain_row(i):
        return gain[pl.ds(i, 1), :]

    def first_norm(at):
        y = rms(tok[at, :].astype(F32)) * gain_row(0)
        xg1[pl.ds(pl.multiple_of(t * rows + at.start, 16), 16), :] = y.astype(BF16)

    with scope("barrier"):
        pl.semaphore_wait(barrier, len(greeted))
    r_in.begin()
    r_out.begin()
    with scope("fetch"):
        fetch.wait()
    with scope("norm0"):
        lines(0, half, first_norm)
    g1.begin(0)
    lines(half, half, first_norm)
    g1.begin(1)
    local = [
        pltpu.make_async_copy(w_in, rows_of(b_in, k_in, 0, k_in)(z), own_sem.at[0]),
        pltpu.make_async_copy(w_out, cols_of(b_out, n_out, 0, k_out)(z), own_sem.at[1]),
        pltpu.make_async_copy(w_up, rows_of(b_up, k_up, 0, k_up)(z), own_sem.at[2]),
        pltpu.make_async_copy(w_down, cols_of(b_down, n_down, 0, f_down)(0), own_sem.at[3]),
    ]
    for copy in local:
        copy.start()
    mixed[pl.ds(0, 16), :] = jnp.zeros((16, mixed.shape[1]), F32)

    pair = 2 * rows

    def chip_rows(chip):
        return pl.ds(pl.multiple_of(chip * pair, 16), pair)

    def rows_at(tp):
        return pl.ds(pl.multiple_of(tp * rows, 16), rows)

    def mix(chip):
        y = jnp.dot(xg1[chip_rows(chip), :], b_in[...], preferred_element_type=F32)
        mixed[pl.ds(pl.multiple_of(chip * pair + 16, 16), pair), :] = y.astype(BF16).astype(F32)

    channels = mixed.shape[1]
    lane = lax.broadcasted_iota(jnp.int32, (1, channels), 1)
    group = (t * channels + lane) // (PW // GROUPS)

    def pick(a, b, c, d):
        return jnp.where(group == 0, a, jnp.where(group == 1, b, jnp.where(group == 2, c, d)))

    span = pick(2, 4, 8, 16)

    def pool(chip):
        for part in (0, 1):
            first = (chip * 2 + part) * rows
            v = mixed[pl.ds(pl.multiple_of(first, 16), rows + 16), :]
            two = v + pltpu.roll(v, 1, 0)
            four = two + pltpu.roll(two, 2, 0)
            eight = four + pltpu.roll(four, 4, 0)
            total = pick(two, four, eight, eight + pltpu.roll(eight, 8, 0))
            total, v = total[16:, :], v[16:, :]
            position = first + 1 + lax.broadcasted_iota(jnp.int32, (rows, channels), 0)
            count = jnp.minimum(position, span).astype(F32)
            y = (total / count - v) * scale[...]
            scaled[rows_at(chip * 2 + part), :] = y.astype(BF16)

    every = pl.ds(0, width)

    def product(left, right, to, at, cols=every, finish=lambda y: y):
        y = jnp.dot(left[at, :], right[:, cols], preferred_element_type=F32)
        to[at, cols] = finish(y).astype(BF16)

    def for_mate(total, left, right, i):
        product(left, right, total.part, rows_at(dest[i] * 2 + 1 - core), total.cols)
        total.give(i)

    def for_me(total, left, right, i):
        product(left, right, total.part, rows_at(dest[i] * 2 + core), total.cols)

    def expand(chip):
        def finish(h):
            h = jnp.maximum(h, 0.0)
            return h * h

        product(xg2, b_up, sq, chip_rows(chip), pl.ds(0, sq.shape[1]), finish)

    def second_norm(at):
        m = tok[at, :].astype(F32) + rms(s1.result(at)) * gain_row(1)
        m = m.astype(BF16)
        mid[at, :] = m
        y = rms(m.astype(F32)) * gain_row(2)
        xg2[pl.ds(pl.multiple_of(t * rows + at.start, 16), 16), :] = y.astype(BF16)

    def middle(h):
        s1.finish(h)
        with scope("norm1"):
            lines(h * half, half, second_norm)
        g2.begin(h)

    def weights_in():
        for copy in local:
            copy.wait()
        r_in.mirrored()
        r_out.mirrored()

    do = functools.partial
    back = (scaled, b_out)
    at_time(12.8, do(g1.near, 0))
    at_time(18.5, do(g1.near, 1))
    at_time(21.5, do(g1.far, 0))
    at_time(24.5, do(g1.far, 1))
    at_time(25.0, weights_in, g1.mate_own, do(mix, x), g1.mate_near, do(mix, chip_r))
    at_time(26.0, do(pool, chip_r), do(for_mate, s1, *back, 1), do(for_me, s1, *back, 1))
    at_time(26.5, do(mix, chip_l), g1.mate_far, do(mix, chip_o), do(pool, chip_o))
    at_time(26.8, do(s1.add, 1), do(s1.direct, 0), do(for_mate, s1, *back, 0))
    at_time(27.5, do(pool, chip_l), do(for_mate, s1, *back, 2), do(for_me, s1, *back, 0))
    at_time(28.0, do(s1.add, 0), do(s1.far, 1), do(s1.far, 0))
    at_time(28.5, do(for_me, s1, *back, 2), do(s1.add, 2), do(s1.direct, 1))
    at_time(29.5, do(pool, x), do(for_mate, s1, *back, 3))
    at_time(30.5, do(for_me, s1, *back, 3))
    at_time(36.2, do(s1.relay, 1, 0))
    at_time(36.4, do(s1.relay, 0, 0), s1.own)
    at_time(38.7, do(s1.relay, 1, 1))
    at_time(39.2, do(s1.relay, 0, 1))
    at_time(46.5, do(middle, 0))
    at_time(49.0, do(middle, 1))
    at_time(56.0, g2.mate_own, do(g2.near, 0))
    at_time(61.5, do(g2.near, 1))
    at_time(62.5, r_uo.mirrored, do(expand, x))
    at_time(63.5, g2.mate_near, do(expand, chip_r))
    at_time(64.5, do(g2.far, 0), do(expand, chip_l))
    at_time(67.0, do(g2.far, 1))
    at_time(68.5, g2.mate_far, do(expand, chip_o))
    back = (sq, b_down)

    for turn, s in enumerate(lasts):
        first, second, third, fourth, fifth, sixth = LAST_TIMES[turn]
        at_time(first, do(r_do.mirrored, turn), do(for_mate, s, *back, 1))
        at_time(first, do(for_me, s, *back, 1), do(for_mate, s, *back, 2))
        at_time(second, do(s.add, 1), do(s.direct, 0), do(for_me, s, *back, 2))
        at_time(third, do(for_mate, s, *back, 0), do(s.add, 2), do(s.direct, 1))
        at_time(fourth, do(for_me, s, *back, 0), do(s.add, 0), do(s.far, 0), do(s.far, 1))
        at_time(fifth, do(for_mate, s, *back, 3), do(for_me, s, *back, 3))
        for k in (0, 1):
            at_time(sixth + 1.5 * k, do(s.relay, 0, k), do(s.relay, 1, k))
    for _, _, step in sorted(due, key=lambda entry: entry[:2]):
        step()
    for s in lasts:
        s.own()
    with scope("drain"):
        for copies in pairs[: -len(lasts)]:
            if copies.size:
                copies.drain(mate)

    def last_norm(at):
        total = lasts[0].result(at)
        scaled_by = lax.rsqrt(jnp.mean(total * total, axis=-1, keepdims=True) + EPS)
        for slot in range(n_fs):
            away = (slot + 1) // 2
            origin = lax.rem(z + (n_fs - away if slot % 2 else away), n_fs)
            cols = pl.ds(pl.multiple_of(origin * n_down, 128), n_down)
            y = total[:, slot * n_down : (slot + 1) * n_down] * scaled_by
            y = mid[at, cols].astype(F32) + y * gain[pl.ds(3, 1), cols]
            last[at, cols] = y.astype(BF16)

    puts = []
    for h in (0, 1):
        for s in lasts:
            s.finish(h)
        with scope("norm3"):
            lines(h * half, half, last_norm)
        at = pl.ds(h * half, half)
        puts.append(pltpu.make_async_copy(last.at[at, :], out.at[at, :], own_sem.at[h]))
        puts[-1].start()
    with scope("end"):
        for copies in c_last:
            copies.drain(mate)
        for put in puts:
            put.wait()


def solution(mesh):
    n_fs, n_tp = mesh.shape["fs"], mesh.shape["tp"]
    paired = mesh.shape["grp"] % 2 == 0

    def layer(tokens, mix_in, pool_scale, mix_out, up, down, gains):
        rows, width = tokens.shape
        channels, hidden = mix_in.shape[1], up.shape[1]
        seq = rows * n_tp
        vmem = pl.BlockSpec(memory_space=pltpu.VMEM)
        far = pl.BlockSpec(memory_space=pl.ANY)
        sems = []
        counts = {"iy": 1, "oy": 1, "uy": 1, "dx": 1, "dy": 1, "dz": 1, "ag": 20, "ah": 20, "rs": 16, "rt": 16, "ru": 16, "rv": 16}
        for name in NAMES:
            sems.append(pltpu.SemaphoreType.DMA((1,)))
            sems.append(pltpu.SemaphoreType.DMA((counts.get(name, n_fs - 1),)))
        sums = lambda *lead: pltpu.VMEM((*lead, width), BF16)
        return pl.pallas_call(
            functools.partial(kernel, (n_fs, n_tp, paired)),
            out_shape=jax.ShapeDtypeStruct((rows, width), BF16),
            in_specs=[far, vmem, vmem, vmem, vmem, far, far],
            out_specs=far,
            scratch_shapes=[
                sums(rows),
                sums(seq), sums(seq),
                pltpu.VMEM((width, channels), BF16),
                sums(channels),
                pltpu.VMEM((width, hidden), BF16),
                sums(hidden),
                pltpu.VMEM((seq + 16, channels), F32),
                pltpu.VMEM((seq, channels), BF16),
                pltpu.VMEM((seq, hidden), BF16),
                sums(rows), sums(rows),
                sums(seq), sums(seq),
                sums(4, rows), sums(4, rows),
                sums(2, rows // 2), sums(2, rows // 2),
                sums(2, rows), sums(2, rows),
                sums(3, rows), sums(3, rows),
                pltpu.SemaphoreType.DMA((5,)),
                *sems,
            ],
            compiler_params=pltpu.CompilerParams(
                collective_id=0,
                has_side_effects=True,
                vmem_limit_bytes=60 * 1024 * 1024,
            ),
            name="layer",
        )(tokens, gains, pool_scale.reshape(1, -1), mix_in, mix_out, up, down)

    spread = P(("grp", "fs", "tp"), None)
    return jax.shard_map(
        layer,
        mesh=mesh,
        in_specs=(
            spread,
            P("fs", "tp"),
            P("tp"),
            P("tp", "fs"),
            P("fs", "tp"),
            P("tp", "fs"),
            P(),
        ),
        out_specs=spread,
        check_vma=False,
    )
```
